32 devices in a mesh: fs: 8 (over z, x), tp: 4 (over y, core).
Axes of the slice: x: 2, y: 2, z: 4, core: 2. Of those that a mesh axis runs over, the one named last changes fastest.
Arguments:
- tokens: bfloat16 [4096, 2048], P(('fs', 'tp')), may hold values from -6 to 6
- gate_weight: bfloat16 [5632, 2048], P('tp', 'fs'), may hold values from -0.125 to 0.125
- up_weight: bfloat16 [5632, 2048], P('tp', 'fs'), may hold values from -0.125 to 0.125
- down_weight: bfloat16 [5632, 2048], P('tp', 'fs'), may hold values from -0.078125 to 0.078125
- out_grad: bfloat16 [4096, 2048], P(('fs', 'tp')), may hold values from -6 to 6
Outputs:
- grad_tokens: bfloat16 [4096, 2048], P(('fs', 'tp'))
- grad_gate: float32 [5632, 2048], P('tp', 'fs')
- grad_up: float32 [5632, 2048], P('tp', 'fs')
- grad_down: float32 [5632, 2048], P('tp', 'fs')
- gate_rows: float32 [5632], P('tp')
- up_rows: float32 [5632], P('tp')
- down_rows: float32 [5632], P('tp')
The draws below stay inside these ranges and needn't reach their ends.
All inputs are finite; a program needn't handle non-finite values.
Results may differ from the reference program's by a relative error of at most 0.014.
Values may be sent and summed in bfloat16 or wider, within the bound.
A program may use at most 128 MiB of HBM per device.

```python
import math
import jax
import jax.numpy as jnp
from jax import lax

D = 2048
FF = 5632
TOKENS = 4096
N_TP = 4


def with_spikes(values, rng, source, target, blocks, factor):
    def block_of(axis_at):
        return (jnp.arange(values.shape[axis_at]) // (values.shape[axis_at] // blocks)).reshape((-1,) + (1,) * (values.ndim - 1 - axis_at))

    near = jax.random.permutation(rng, blocks)[block_of(target)]
    other_side = (block_of(target) + blocks // 2) % blocks
    return jnp.where((block_of(source) == near) | (block_of(source) == other_side), factor * values, values)


def block_levels(own_key, shape, split, low, high):
    factor_of = 1.0
    for position, parts in split:
        steps = jax.random.uniform(jax.random.fold_in(jax.random.fold_in(own_key, 6), position), (parts,), jnp.float32, low / len(split), high / len(split))
        factor_of = factor_of * jnp.repeat(jnp.exp(steps), shape[position] // parts).reshape((-1,) + (1,) * (len(shape) - 1 - position))
    return factor_of


def noise(key, dims, scale, most, shards=(), dtype=jnp.bfloat16):
    values = scale * jax.random.normal(key, dims, jnp.float32)
    if shards:
        values = values * block_levels(key, dims, shards, -0.22, 0.18)
    return jnp.clip(values, -most, most).astype(dtype)


def bell_draw_with(stream_key, shape, scale, limit, pieces, heavy, held_as=jnp.bfloat16):
    values = scale * jax.random.normal(stream_key, shape, jnp.float32)
    if pieces:
        values = values * block_levels(stream_key, shape, pieces, -0.22, 0.18)
    return jnp.clip(with_spikes(values, jax.random.fold_in(stream_key, 3), *heavy), -limit, limit).astype(held_as)


def setup_inputs(seed: int = 0) -> dict:
    keys = jax.random.split(jax.random.key(seed), 6)
    tokens = noise(keys[0], (TOKENS, D), 1.0, 6.0, ((0, 32),))
    gate_weight = noise(keys[1], (FF, D), D ** -0.5, 0.125, ((0, 4), (1, 8)))
    up_weight = noise(keys[2], (FF, D), D ** -0.5, 0.125, ((0, 4), (1, 8)))
    down_weight = noise(keys[3], (FF, D), FF ** -0.5, 0.078125, ((0, 4), (1, 8)))
    out_grad = bell_draw_with(keys[4], (TOKENS, D), 1.0, 6.0, ((0, 32),), (0, 1, 32, 2.75))
    return {"tokens": tokens, "gate_weight": gate_weight, "up_weight": up_weight, "down_weight": down_weight, "out_grad": out_grad}


def reference(tokens, gate_weight, up_weight, down_weight, out_grad):
    gate = jnp.dot(tokens, gate_weight.T, preferred_element_type=jnp.float32)
    up = jnp.dot(tokens, up_weight.T, preferred_element_type=jnp.float32)
    sig = jax.nn.sigmoid(gate)
    silu = gate * sig
    act = (silu * up).astype(jnp.bfloat16)
    dhidden = jnp.dot(out_grad, down_weight.T, preferred_element_type=jnp.float32)
    dgate = (dhidden * up * sig * (1.0 + gate * (1.0 - sig))).astype(jnp.bfloat16)
    dup = (dhidden * silu).astype(jnp.bfloat16)
    width = FF // N_TP
    total = jnp.zeros((TOKENS, D), jnp.float32)
    for block in range(N_TP):
        lo = block * width
        part = jnp.dot(dgate[:, lo:lo + width], gate_weight[lo:lo + width], preferred_element_type=jnp.float32)
        part = part + jnp.dot(dup[:, lo:lo + width], up_weight[lo:lo + width], preferred_element_type=jnp.float32)
        total = total + lax.optimization_barrier(part.astype(jnp.bfloat16)).astype(jnp.float32)
    grad_tokens = total.astype(jnp.bfloat16)
    factor = 1.0 / math.sqrt(TOKENS)
    grad_gate = jnp.dot(dgate.T, tokens, preferred_element_type=jnp.float32) * factor
    grad_up = jnp.dot(dup.T, tokens, preferred_element_type=jnp.float32) * factor
    grad_down = jnp.dot(act.T, out_grad, preferred_element_type=jnp.float32) * factor
    gate_rows = lax.optimization_barrier(jnp.mean(grad_gate * grad_gate, axis=1))
    up_rows = lax.optimization_barrier(jnp.mean(grad_up * grad_up, axis=1))
    down_rows = lax.optimization_barrier(jnp.mean(grad_down * grad_down, axis=1))
    return (grad_tokens, grad_gate, grad_up, grad_down, gate_rows, up_rows, down_rows)
```

```python
import math

import jax
import jax.numpy as jnp
from jax import lax
from jax.sharding import PartitionSpec as P


BF, F32 = jnp.bfloat16, jnp.float32


def split_sizes(fs, tp):
    nx = max(d for d in range(1, fs + 1) if fs % d == 0 and d * d <= fs)
    nc = 2 if tp % 2 == 0 else 1
    return fs // nx, nx, tp // nc, nc


def make_body(fs, tp):
    nz, nx, ny, nc = split_sizes(fs, tp)

    def shift_z(v, k):
        return lax.ppermute(v, "fs", [(a * nx + b, (a + k) % nz * nx + b) for a in range(nz) for b in range(nx)])

    def step_z(v, k):
        pairs = [(a * nx + b, (a + k) * nx + b) for a in range(nz) for b in range(nx) if 0 <= a + k < nz]
        return lax.ppermute(v, "fs", pairs)

    def shift_x(v, k):
        return lax.ppermute(v, "fs", [(a * nx + b, a * nx + (b + k) % nx) for a in range(nz) for b in range(nx)])

    def shift_y(v, k):
        return lax.ppermute(v, "tp", [(a * nc + b, (a + k) % ny * nc + b) for a in range(ny) for b in range(nc)])

    def shift_c(v, k):
        return lax.ppermute(v, "tp", [(a * nc + b, a * nc + (b + k) % nc) for a in range(ny) for b in range(nc)])

    def gather_rows(v, z):
        up, down = [v], [v]
        for _ in range(nz - 1):
            up.append(step_z(up[-1], 1))
            down.append(step_z(down[-1], -1))
        held = [v] + [jnp.where(z >= k, up[k], down[nz - k]) for k in range(1, nz)]
        out = []
        for k in range(nz):
            across = [held[k]] + [shift_y(held[k], j) for j in range(1, ny)]
            for piece in across:
                out.append(piece)
                out.extend(shift_c(piece, i) for i in range(1, nc))
        return jnp.concatenate(out, axis=0)

    def place(pieces, at, axis):
        n = len(pieces)
        ring = [pieces[-j % n] for j in range(n)]
        both = jnp.stack(ring + ring[:-1], axis=axis)
        return lax.dynamic_slice_in_dim(both, (n - at) % n, n, axis)

    def relative(v, at, axis):
        n = v.shape[axis]
        both = jnp.concatenate([v, lax.slice_in_dim(v, 0, n - 1, axis=axis)], axis)
        return lax.dynamic_slice_in_dim(both, at, n, axis)

    def body(tokens, gate_weight, up_weight, down_weight, out_grad):
        z, x = lax.axis_index("fs") // nx, lax.axis_index("fs") % nx
        rows, width = tokens.shape
        hid, cols = gate_weight.shape
        mine = hid // nz
        inputs = gather_rows(tokens, z)
        cotangent = gather_rows(out_grad, z)

        def gather_weight(w):
            blocks = relative(w.reshape(nz, mine, cols), z, 0)
            got = [blocks[0]] + [shift_z(blocks[k], k) for k in range(1, nz)]
            lines = []
            for piece in got:
                line = [piece] + [shift_x(piece, j) for j in range(1, nx)]
                lines.append(place(line, x, 1))
            return place(lines, z, 1).reshape(mine, width)

        w_gate, w_up, w_down = gather_weight(gate_weight), gather_weight(up_weight), gather_weight(down_weight)
        inner = (((1,), (1,)), ((), ()))
        gate = lax.dot_general(inputs, w_gate, inner, preferred_element_type=F32)
        up = lax.dot_general(inputs, w_up, inner, preferred_element_type=F32)
        dhidden = lax.dot_general(cotangent, w_down, inner, preferred_element_type=F32)
        sig = jax.nn.sigmoid(gate)
        silu = gate * sig
        act = (silu * up).astype(BF)
        dgate = (dhidden * up * sig * (1.0 + gate * (1.0 - sig))).astype(BF)
        dup = (dhidden * silu).astype(BF)
        factor = 1.0 / math.sqrt(rows * fs * tp)
        outer = (((0,), (0,)), ((), ()))

        def weight_grad(left, right):
            part = lax.dot_general(left, right, outer, preferred_element_type=F32) * factor
            part = relative(part.reshape(mine, nz, nx, cols), x, 2)
            total = part[:, :, 0]
            for k in range(1, nx):
                total = total + shift_x(part[:, :, k].astype(BF), k).astype(F32)
            total = total.astype(BF)
            wide = total.astype(F32)
            squares = jnp.sum(wide * wide, axis=(1, 2))
            blocks = relative(total, z, 1)
            got = [blocks[:, 0]] + [shift_z(blocks[:, k], k) for k in range(1, nz)]
            grad = place(got, z, 0).reshape(hid, cols).astype(F32)
            return grad, squares

        grad_down, sq_down = weight_grad(act, cotangent)
        grad_gate, sq_gate = weight_grad(dgate, inputs)
        grad_up, sq_up = weight_grad(dup, inputs)

        squares = jnp.stack([sq_gate, sq_up, sq_down])
        total = squares
        for k in range(1, nx):
            total = total + shift_x(squares, k)
        got = [total] + [shift_z(total, k) for k in range(1, nz)]
        means = place(got, z, 1).reshape(3, hid) / width

        part = jnp.dot(dgate, w_gate, preferred_element_type=F32)
        part = part + jnp.dot(dup, w_up, preferred_element_type=F32)
        part = part.reshape(nz, ny, nc, rows, width)
        total = part[:, :, 0]
        for k in range(1, nc):
            total = total + shift_c(part[:, :, k].astype(BF), -k).astype(F32)
        part, total = total, total[:, 0]
        for k in range(1, ny):
            total = total + shift_y(part[:, k].astype(BF), -k).astype(F32)
        part, total = total, total[0]
        for k in range(1, nz):
            total = total + shift_z(part[k].astype(BF), -k).astype(F32)
        return (total.astype(BF), grad_gate, grad_up, grad_down, means[0], means[1], means[2])

    return body


def solution(mesh):
    return jax.shard_map(
        make_body(mesh.shape["fs"], mesh.shape["tp"]),
        mesh=mesh,
        in_specs=(P(("fs", "tp"), None), P("tp", "fs"), P("tp", "fs"), P("tp", "fs"), P(("fs", "tp"), None)),
        out_specs=(
            P(("fs", "tp"), None),
            P("tp", "fs"),
            P("tp", "fs"),
            P("tp", "fs"),
            P("tp"),
            P("tp"),
            P("tp"),
        ),
        check_vma=False,
    )
```

```python
import functools
import math

import jax
import jax.numpy as jnp
from jax import lax
from jax.experimental import pallas as pl
from jax.experimental.pallas import tpu as pltpu
from jax.sharding import PartitionSpec as P


BF, F32 = jnp.bfloat16, jnp.float32
MESH = pl.DeviceIdType.MESH


def split_sizes(fs, tp):
    nx = max(d for d in range(1, fs + 1) if fs % d == 0 and d * d <= fs)
    nc = 2 if tp % 2 == 0 else 1
    return fs // nx, nx, tp // nc, nc


def gather_kernel(sizes, *refs):
    nz, nx, ny, nc = sizes
    rows_in, weights_in = refs[:2], refs[2:5]
    rows_out, weights_out = refs[5:7], refs[7:10]
    (row_stage, weight_stage, local, zs, zr, ys, yr, cs, cr, ws, wr, xs, xr) = refs[10:]
    fs, tp = lax.axis_index("fs"), lax.axis_index("tp")
    z, x, y, c = fs // nx, fs % nx, tp // nc, tp % nc
    rows = rows_in[0].shape[0]
    hid, cols = weights_in[0].shape
    mine = hid // nz

    def back(at, k, n):
        return lax.rem(at - k + n, n)

    def ahead(at, k, n):
        return lax.rem(at + k, n)

    def dev(dz=0, dx=0, dy=0, dc=0):
        return {
            "fs": ahead(z, dz, nz) * nx + ahead(x, dx, nx),
            "tp": ahead(y, dy, ny) * nc + ahead(c, dc, nc),
        }

    barrier = pltpu.get_barrier_semaphore()
    peers = [dev(dz=k) for k in range(1, nz)] + [dev(dx=k) for k in range(1, nx)]
    peers += [dev(dy=k) for k in range(1, ny)] + [dev(dc=k) for k in range(1, nc)]
    for peer in peers:
        pl.semaphore_signal(barrier, inc=1, device_id=peer, device_id_type=MESH)
    pl.semaphore_wait(barrier, len(peers))

    sent = []

    def when(cond, do):
        if cond is None:
            do()
        else:
            pl.when(cond)(do)

    def make(src, dst, send, recv, to):
        return pltpu.make_async_remote_copy(
            src_ref=src, dst_ref=dst, send_sem=send, recv_sem=recv, device_id=to, device_id_type=MESH
        )

    def go(cond, copy):
        when(cond, copy.start)
        sent.append((cond, copy))

    def slot(a, s, yy, cc):
        at = pl.multiple_of(((s * ny + yy) * nc + cc) * rows, rows)
        return rows_out[a].at[pl.ds(at, rows), :]

    def block(i, zz):
        return weights_in[i].at[pl.ds(pl.multiple_of(zz * mine, mine), mine), :]

    def columns(i, zz, xx):
        at = pl.multiple_of((zz * nx + xx) * cols, cols)
        return weights_out[i].at[:, pl.ds(at, cols)]

    def shards(k):
        if k == 0:
            return [(None, z)]
        return [(z >= k, back(z, k, nz)), (z + k < nz, ahead(z, k, nz))]

    def both(one, two):
        return two if one is None else one & two

    def send_z(a, s, cond, src, way):
        dst = slot(a, s, y, c)
        edge = (z < nz - 1) if way == 1 else (z > 0)
        to = dev(dz=1 if way == 1 else nz - 1)
        go(both(cond, edge), make(src, dst, zs.at[a, s, (way + 1) // 2], zr.at[a, s], to))

    def send_c(a, s, cond, src, j):
        dst = slot(a, s, back(y, j, ny), c)
        for i in range(1, nc):
            go(cond, make(src, dst, cs.at[a, s, j, i], cr.at[a, s, j, i], dev(dc=i)))

    def send_y(a, s, cond, src):
        for j in range(1, ny):
            go(cond, make(src, slot(a, s, y, c), ys.at[a, s, j], yr.at[a, s, j], dev(dy=j)))

    def relay_y(k):
        for a in range(2):
            for cond, s in shards(k):
                for j in range(1, ny):
                    at = slot(a, s, back(y, j, ny), c)
                    when(cond, make(at, at, ys.at[a, s, j], yr.at[a, s, j], dev(dy=j)).wait_recv)
                    send_c(a, s, cond, at, j)

    def send_x(i, k, src):
        dst = columns(i, back(z, k, nz), x)
        for j in range(1, nx):
            go(None, make(src, dst, xs.at[i, k, j], xr.at[i, k, j], dev(dx=j)))

    for a in range(2):
        send_z(a, z, None, rows_in[a], 1)
        send_z(a, z, None, rows_in[a], -1)
    for a in range(2):
        send_y(a, z, None, rows_in[a])
    for i in range(3):
        send_x(i, 0, block(i, z))
    for k in range(1, nz):
        for i in range(3):
            go(None, make(block(i, ahead(z, k, nz)), columns(i, z, x), ws.at[i, k], wr.at[i, k], dev(dz=k)))
    for a in range(2):
        send_c(a, z, None, rows_in[a], 0)

    takes = [pltpu.make_async_copy(rows_in[a], row_stage.at[a], local.at[a]) for a in range(2)]
    takes += [pltpu.make_async_copy(block(i, z), weight_stage.at[i], local.at[2 + i]) for i in range(3)]
    gives = [pltpu.make_async_copy(row_stage.at[a], slot(a, z, y, c), local.at[5 + a]) for a in range(2)]
    gives += [pltpu.make_async_copy(weight_stage.at[i], columns(i, z, x), local.at[7 + i]) for i in range(3)]
    for take in takes:
        take.start()
    for take, give in zip(takes, gives):
        take.wait()
        give.start()

    for k in range(1, nz):
        for a in range(2):
            for way, (cond, s) in zip((1, -1), shards(k)):
                at = slot(a, s, y, c)
                when(cond, make(at, at, zs.at[a, s, 0], zr.at[a, s], dev(dz=1)).wait_recv)
                if k < nz - 1:
                    send_z(a, s, cond, at, way)
                send_y(a, s, cond, at)
                send_c(a, s, cond, at, 0)
        relay_y(k - 1)
        for i in range(3):
            at = columns(i, back(z, k, nz), x)
            make(at, at, ws.at[i, k], wr.at[i, k], dev(dz=k)).wait_recv()
            send_x(i, k, at)
    relay_y(nz - 1)

    for k in range(nz):
        for a in range(2):
            for cond, s in shards(k):
                for j in range(ny):
                    for i in range(1, nc):
                        at = slot(a, s, back(y, j, ny), back(c, i, nc))
                        when(cond, make(at, at, cs.at[a, s, j, i], cr.at[a, s, j, i], dev(dc=i)).wait_recv)
        for i in range(3):
            for j in range(1, nx):
                at = columns(i, back(z, k, nz), back(x, j, nx))
                make(at, at, xs.at[i, k, j], xr.at[i, k, j], dev(dx=j)).wait_recv()
    for cond, copy in sent:
        when(cond, copy.wait_send)
    for give in gives:
        give.wait()


def gather_all(sizes, tokens, out_grad, weights):
    nz, nx, ny, nc = sizes
    rows, width = tokens.shape
    hid, cols = weights[0].shape
    mine = hid // nz
    dma = pltpu.SemaphoreType.DMA
    any_space = pl.BlockSpec(memory_space=pl.ANY)
    return pl.pallas_call(
        functools.partial(gather_kernel, sizes),
        out_shape=[jax.ShapeDtypeStruct((nz * ny * nc * rows, width), BF)] * 2
        + [jax.ShapeDtypeStruct((mine, width), BF)] * 3,
        in_specs=[any_space] * 5,
        out_specs=[any_space] * 5,
        scratch_shapes=[
            pltpu.VMEM((2, rows, width), BF),
            pltpu.VMEM((3, mine, cols), BF),
            dma((10,)),
            dma((2, nz, 2)),
            dma((2, nz)),
            dma((2, nz, ny)),
            dma((2, nz, ny)),
            dma((2, nz, ny, nc)),
            dma((2, nz, ny, nc)),
            dma((3, nz)),
            dma((3, nz)),
            dma((3, nz, nx)),
            dma((3, nz, nx)),
        ],
        compiler_params=pltpu.CompilerParams(collective_id=0, has_side_effects=True),
    )(tokens, out_grad, *weights)


def make_body(fs, tp):
    nz, nx, ny, nc = split_sizes(fs, tp)

    def shift_z(v, k):
        return lax.ppermute(v, "fs", [(a * nx + b, (a + k) % nz * nx + b) for a in range(nz) for b in range(nx)])

    def shift_x(v, k):
        return lax.ppermute(v, "fs", [(a * nx + b, a * nx + (b + k) % nx) for a in range(nz) for b in range(nx)])

    def shift_y(v, k):
        return lax.ppermute(v, "tp", [(a * nc + b, (a + k) % ny * nc + b) for a in range(ny) for b in range(nc)])

    def shift_c(v, k):
        return lax.ppermute(v, "tp", [(a * nc + b, a * nc + (b + k) % nc) for a in range(ny) for b in range(nc)])

    def place(pieces, at, axis):
        n = len(pieces)
        ring = [pieces[-j % n] for j in range(n)]
        both = jnp.stack(ring + ring[:-1], axis=axis)
        return lax.dynamic_slice_in_dim(both, (n - at) % n, n, axis)

    def pick(v, at, k, axis):
        n = v.shape[axis]
        return lax.dynamic_index_in_dim(v, (at + k) % n, axis, keepdims=False)

    def body(tokens, gate_weight, up_weight, down_weight, out_grad):
        fs_at, tp_at = lax.axis_index("fs"), lax.axis_index("tp")
        z, x, y, c = fs_at // nx, fs_at % nx, tp_at // nc, tp_at % nc
        rows, width = tokens.shape
        hid, cols = gate_weight.shape
        mine = hid // nz
        inputs, cotangent, w_gate, w_up, w_down = gather_all(
            (nz, nx, ny, nc), tokens, out_grad, (gate_weight, up_weight, down_weight)
        )
        inner = (((1,), (1,)), ((), ()))
        gate = lax.dot_general(inputs, w_gate, inner, preferred_element_type=F32)
        up = lax.dot_general(inputs, w_up, inner, preferred_element_type=F32)
        dhidden = lax.dot_general(cotangent, w_down, inner, preferred_element_type=F32)
        sig = jax.nn.sigmoid(gate)
        silu = gate * sig
        act = (silu * up).astype(BF)
        dgate = (dhidden * up * sig * (1.0 + gate * (1.0 - sig))).astype(BF)
        dup = (dhidden * silu).astype(BF)
        factor = 1.0 / math.sqrt(rows * fs * tp)
        outer = (((0,), (0,)), ((), ()))

        def weight_grad(left, right):
            part = lax.dot_general(left, right, outer, preferred_element_type=F32) * factor
            part = part.reshape(mine, nz, nx, cols)
            total = pick(part, x, 0, 2)
            for k in range(1, nx):
                total = total + shift_x(pick(part, x, k, 2).astype(BF), k).astype(F32)
            total = total.astype(BF)
            wide = total.astype(F32)
            squares = jnp.sum(wide * wide, axis=(1, 2))
            got = [pick(total, z, 0, 1)] + [shift_z(pick(total, z, k, 1), k) for k in range(1, nz)]
            grad = place(got, z, 0).reshape(hid, cols).astype(F32)
            return grad, squares

        grad_down, sq_down = weight_grad(act, cotangent)
        grad_gate, sq_gate = weight_grad(dgate, inputs)
        grad_up, sq_up = weight_grad(dup, inputs)

        squares = jnp.stack([sq_gate, sq_up, sq_down])
        total = squares
        for k in range(1, nx):
            total = total + shift_x(squares, k)
        got = [total] + [shift_z(total, k) for k in range(1, nz)]
        means = place(got, z, 1).reshape(3, hid) / width

        part = jnp.dot(dgate, w_gate, preferred_element_type=F32)
        part = part + jnp.dot(dup, w_up, preferred_element_type=F32)
        part = part.reshape(nz, ny, nc, rows, width)
        total = pick(part, c, 0, 2)
        for k in range(1, nc):
            total = total + shift_c(pick(part, c, k, 2).astype(BF), k).astype(F32)
        part, total = total, pick(total, y, 0, 1)
        for k in range(1, ny):
            total = total + shift_y(pick(part, y, k, 1).astype(BF), k).astype(F32)
        part, total = total, pick(total, z, 0, 0)
        for k in range(1, nz):
            total = total + shift_z(pick(part, z, k, 0).astype(BF), k).astype(F32)
        return (total.astype(BF), grad_gate, grad_up, grad_down, means[0], means[1], means[2])

    return body


def solution(mesh):
    return jax.shard_map(
        make_body(mesh.shape["fs"], mesh.shape["tp"]),
        mesh=mesh,
        in_specs=(P(("fs", "tp"), None), P("tp", "fs"), P("tp", "fs"), P("tp", "fs"), P(("fs", "tp"), None)),
        out_specs=(
            P(("fs", "tp"), None),
            P("tp", "fs"),
            P("tp", "fs"),
            P("tp", "fs"),
            P("tp"),
            P("tp"),
            P("tp"),
        ),
        check_vma=False,
    )
```

```python
import functools
import math

import jax
import jax.numpy as jnp
from jax import lax
from jax.experimental import pallas as pl
from jax.experimental.pallas import tpu as pltpu
from jax.sharding import PartitionSpec as P

BF, F32 = jnp.bfloat16, jnp.float32
MESH = pl.DeviceIdType.MESH


def split_sizes(fs, tp):
    nx = max(d for d in range(1, fs + 1) if fs % d == 0 and d * d <= fs)
    nc = 2 if tp % 2 == 0 else 1
    return fs // nx, nx, tp // nc, nc


def gather_kernel(sizes, *refs):
    nz, nx, ny, nc = sizes
    rows_in, weights_in = refs[:2], refs[2:5]
    rows_out, weights_out = refs[5:7], refs[7:10]
    (row_stage, weight_stage, local, zs, zr, ys, yr, cs, cr, ws, wr, xs, xr) = refs[10:]
    fs, tp = lax.axis_index("fs"), lax.axis_index("tp")
    z, x, y, c = fs // nx, fs % nx, tp // nc, tp % nc
    rows = rows_in[0].shape[0]
    hid, cols = weights_in[0].shape
    mine = hid // nz

    def back(at, k, n):
        return lax.rem(at - k + n, n)

    def ahead(at, k, n):
        return lax.rem(at + k, n)

    def dev(dz=0, dx=0, dy=0, dc=0):
        return {
            "fs": ahead(z, dz, nz) * nx + ahead(x, dx, nx),
            "tp": ahead(y, dy, ny) * nc + ahead(c, dc, nc),
        }

    barrier = pltpu.get_barrier_semaphore()
    peers = [dev(dz=k) for k in range(1, nz)] + [dev(dx=k) for k in range(1, nx)]
    peers += [dev(dy=k) for k in range(1, ny)] + [dev(dc=k) for k in range(1, nc)]
    for peer in peers:
        pl.semaphore_signal(barrier, inc=1, device_id=peer, device_id_type=MESH)
    pl.semaphore_wait(barrier, len(peers))

    sent = []

    def when(cond, do):
        if cond is None:
            do()
        else:
            pl.when(cond)(do)

    def make(src, dst, send, recv, to):
        return pltpu.make_async_remote_copy(
            src_ref=src, dst_ref=dst, send_sem=send, recv_sem=recv, device_id=to, device_id_type=MESH
        )

    def go(cond, copy):
        when(cond, copy.start)
        sent.append((cond, copy))

    def slot(a, s, yy, cc):
        at = pl.multiple_of(((s * ny + yy) * nc + cc) * rows, rows)
        return rows_out[a].at[pl.ds(at, rows), :]

    def block(i, zz):
        return weights_in[i].at[pl.ds(pl.multiple_of(zz * mine, mine), mine), :]

    def columns(i, zz, xx):
        at = pl.multiple_of((zz * nx + xx) * cols, cols)
        return weights_out[i].at[:, pl.ds(at, cols)]

    def shards(k):
        if k == 0:
            return [(None, z)]
        return [(z >= k, back(z, k, nz)), (z + k < nz, ahead(z, k, nz))]

    def both(one, two):
        return two if one is None else one & two

    def send_z(a, s, cond, src, way):
        dst = slot(a, s, y, c)
        edge = (z < nz - 1) if way == 1 else (z > 0)
        to = dev(dz=1 if way == 1 else nz - 1)
        go(both(cond, edge), make(src, dst, zs.at[a, s, (way + 1) // 2], zr.at[a, s], to))

    def send_c(a, s, cond, src, j):
        dst = slot(a, s, back(y, j, ny), c)
        for i in range(1, nc):
            go(cond, make(src, dst, cs.at[a, s, j, i], cr.at[a, s, j, i], dev(dc=i)))

    def send_y(a, s, cond, src):
        for j in range(1, ny):
            go(cond, make(src, slot(a, s, y, c), ys.at[a, s, j], yr.at[a, s, j], dev(dy=j)))

    def relay_y(k):
        for a in range(2):
            for cond, s in shards(k):
                for j in range(1, ny):
                    at = slot(a, s, back(y, j, ny), c)
                    when(cond, make(at, at, ys.at[a, s, j], yr.at[a, s, j], dev(dy=j)).wait_recv)
                    send_c(a, s, cond, at, j)

    def send_x(i, k, src):
        dst = columns(i, back(z, k, nz), x)
        for j in range(1, nx):
            go(None, make(src, dst, xs.at[i, k, j], xr.at[i, k, j], dev(dx=j)))

    for a in range(2):
        send_z(a, z, None, rows_in[a], 1)
        send_z(a, z, None, rows_in[a], -1)
    for a in range(2):
        send_y(a, z, None, rows_in[a])
    for i in range(3):
        send_x(i, 0, block(i, z))
    for k in range(1, nz):
        for i in range(3):
            go(None, make(block(i, ahead(z, k, nz)), columns(i, z, x), ws.at[i, k], wr.at[i, k], dev(dz=k)))
    for a in range(2):
        send_c(a, z, None, rows_in[a], 0)

    takes = [pltpu.make_async_copy(rows_in[a], row_stage.at[a], local.at[a]) for a in range(2)]
    takes += [pltpu.make_async_copy(block(i, z), weight_stage.at[i], local.at[2 + i]) for i in range(3)]
    gives = [pltpu.make_async_copy(row_stage.at[a], slot(a, z, y, c), local.at[5 + a]) for a in range(2)]
    gives += [pltpu.make_async_copy(weight_stage.at[i], columns(i, z, x), local.at[7 + i]) for i in range(3)]
    for take in takes:
        take.start()
    for take, give in zip(takes, gives):
        take.wait()
        give.start()

    for k in range(1, nz):
        for a in range(2):
            for way, (cond, s) in zip((1, -1), shards(k)):
                at = slot(a, s, y, c)
                when(cond, make(at, at, zs.at[a, s, 0], zr.at[a, s], dev(dz=1)).wait_recv)
                if k < nz - 1:
                    send_z(a, s, cond, at, way)
                send_y(a, s, cond, at)
                send_c(a, s, cond, at, 0)
        relay_y(k - 1)
        for i in range(3):
            at = columns(i, back(z, k, nz), x)
            make(at, at, ws.at[i, k], wr.at[i, k], dev(dz=k)).wait_recv()
            send_x(i, k, at)
    relay_y(nz - 1)

    for k in range(nz):
        for a in range(2):
            for cond, s in shards(k):
                for j in range(ny):
                    for i in range(1, nc):
                        at = slot(a, s, back(y, j, ny), back(c, i, nc))
                        when(cond, make(at, at, cs.at[a, s, j, i], cr.at[a, s, j, i], dev(dc=i)).wait_recv)
        for i in range(3):
            for j in range(1, nx):
                at = columns(i, back(z, k, nz), back(x, j, nx))
                make(at, at, xs.at[i, k, j], xr.at[i, k, j], dev(dx=j)).wait_recv()
    for cond, copy in sent:
        when(cond, copy.wait_send)
    for give in gives:
        give.wait()


def gather_all(sizes, tokens, out_grad, weights):
    nz, nx, ny, nc = sizes
    rows, width = tokens.shape
    hid, cols = weights[0].shape
    mine = hid // nz
    dma = pltpu.SemaphoreType.DMA
    any_space = pl.BlockSpec(memory_space=pl.ANY)
    return pl.pallas_call(
        functools.partial(gather_kernel, sizes),
        out_shape=[jax.ShapeDtypeStruct((nz * ny * nc * rows, width), BF)] * 2
        + [jax.ShapeDtypeStruct((mine, width), BF)] * 3,
        in_specs=[any_space] * 5,
        out_specs=[any_space] * 5,
        scratch_shapes=[
            pltpu.VMEM((2, rows, width), BF),
            pltpu.VMEM((3, mine, cols), BF),
            dma((10,)),
            dma((2, nz, 2)),
            dma((2, nz)),
            dma((2, nz, ny)),
            dma((2, nz, ny)),
            dma((2, nz, ny, nc)),
            dma((2, nz, ny, nc)),
            dma((3, nz)),
            dma((3, nz)),
            dma((3, nz, nx)),
            dma((3, nz, nx)),
        ],
        compiler_params=pltpu.CompilerParams(collective_id=0, has_side_effects=True),
    )(tokens, out_grad, *weights)


def reduce_kernel(sizes, *refs):
    nz, nx, ny, nc = sizes
    part, grads = refs[0], refs[1:4]
    out_rows, out_grads, out_squares = refs[4:7]
    (crecv, csum, yrecv, ysum, zrecv, xrecv, xsum, qsum, qrecv) = refs[7:16]
    (cs, cr, ys, yr, zs, zr, xs, xr, ws, wr, qxs, qxr, qzs, qzr) = refs[16:]
    fs, tp = lax.axis_index("fs"), lax.axis_index("tp")
    z, x, y, c = fs // nx, fs % nx, tp // nc, tp % nc
    mine, width = grads[0].shape
    cols = width // (nz * nx)

    def back(at, k, n):
        return lax.rem(at - k + n, n)

    def ahead(at, k, n):
        return lax.rem(at + k, n)

    def dev(dz=0, dx=0, dy=0, dc=0):
        return {
            "fs": ahead(z, dz, nz) * nx + ahead(x, dx, nx),
            "tp": ahead(y, dy, ny) * nc + ahead(c, dc, nc),
        }

    barrier = pltpu.get_barrier_semaphore()
    peers = [dev(dz=k) for k in range(1, nz)] + [dev(dx=k) for k in range(1, nx)]
    peers += [dev(dy=k) for k in range(1, ny)] + [dev(dc=k) for k in range(1, nc)]
    for peer in peers:
        pl.semaphore_signal(barrier, inc=1, device_id=peer, device_id_type=MESH)
    pl.semaphore_wait(barrier, len(peers))

    sent = []

    def make(src, dst, send, recv, to):
        return pltpu.make_async_remote_copy(
            src_ref=src, dst_ref=dst, send_sem=send, recv_sem=recv, device_id=to, device_id_type=MESH
        )

    def go(copy):
        copy.start()
        sent.append(copy)

    def columns(i, zz, xx):
        at = pl.multiple_of((zz * nx + xx) * cols, cols)
        return grads[i].at[:, pl.ds(at, cols)]

    def ccopy(k, m, i):
        s, yy = ahead(z, k, nz), ahead(y, m, ny)
        return make(part.at[s, yy, ahead(c, i, nc)], crecv.at[s, yy, i], cs.at[k, m, i], cr.at[s, yy, i], dev(dc=i))

    def ycopy(k, m):
        s = ahead(z, k, nz)
        return make(csum.at[s, ahead(y, m, ny)], yrecv.at[s, m], ys.at[k, m], yr.at[s, m], dev(dy=m))

    def zcopy(k):
        return make(ysum.at[ahead(z, k, nz)], zrecv.at[k], zs.at[k], zr.at[k], dev(dz=k))

    def xcopy(i, k, j):
        zz = ahead(z, k, nz)
        return make(columns(i, zz, ahead(x, j, nx)), xrecv.at[i, zz, j], xs.at[i, k, j], xr.at[i, k, j], dev(dx=j))

    def wcopy(i, k):
        at = pl.ds(pl.multiple_of(z * mine, mine), mine)
        return make(xsum.at[i, ahead(z, k, nz)], out_grads.at[i, at, :], ws.at[i, k], wr.at[i, k], dev(dz=k))

    order = list(range(nz - 1, 0, -1)) + [0]
    for k in order:
        for m in list(range(1, ny)) + [0]:
            for i in range(1, nc):
                go(ccopy(k, m, i))
    for k in order:
        for i in range(3):
            for j in range(1, nx):
                go(xcopy(i, k, j))
    for k in order:
        s = ahead(z, k, nz)
        for m in list(range(1, ny)) + [0]:
            yy = ahead(y, m, ny)
            total = part[s, yy, c].astype(F32)
            for i in range(1, nc):
                ccopy(k, m, i).wait_recv()
                total = total + crecv[s, yy, i].astype(F32)
            csum[s, yy] = total.astype(BF)
            if m > 0:
                go(ycopy(k, m))
    ones = jnp.ones((8, cols), F32)
    for k in order:
        zz = ahead(z, k, nz)
        for i in range(3):
            total = columns(i, zz, x)[...].astype(F32)
            for j in range(1, nx):
                xcopy(i, k, j).wait_recv()
                total = total + xrecv[i, zz, j].astype(F32)
            total = total.astype(BF)
            if k > 0:
                xsum[i, zz] = total
                go(wcopy(i, k))
            else:
                out_grads[i, pl.ds(pl.multiple_of(z * mine, mine), mine), :] = total
            wide = total.astype(F32)
            squares = lax.dot_general(
                ones, wide * wide, (((1,), (1,)), ((), ())), precision=lax.Precision.HIGHEST, preferred_element_type=F32
            )
            if k == order[0]:
                qsum[i] = squares
            else:
                qsum[i] += squares
        total = csum[zz, y].astype(F32)
        for m in range(1, ny):
            ycopy(k, m).wait_recv()
            total = total + yrecv[zz, m].astype(F32)
        ysum[zz] = total.astype(BF)
        if k > 0:
            go(zcopy(k))

    def qxcopy(j):
        return make(qsum, qrecv.at[j], qxs.at[j], qxr.at[j], dev(dx=j))

    def qzcopy(k):
        return make(qrecv.at[0], out_squares.at[z], qzs.at[k], qzr.at[k], dev(dz=k))

    for j in range(1, nx):
        go(qxcopy(j))
    total = qsum[...]
    for j in range(1, nx):
        qxcopy(j).wait_recv()
        total = total + qrecv[j]
    qrecv[0] = total
    out_squares[z] = total
    for k in range(1, nz):
        go(qzcopy(k))

    total = ysum[z].astype(F32)
    for k in order[:-1]:
        zcopy(k).wait_recv()
        total = total + zrecv[k].astype(F32)
    out_rows[...] = total.astype(BF)
    for k in range(1, nz):
        for i in range(3):
            at = pl.ds(pl.multiple_of(back(z, k, nz) * mine, mine), mine)
            make(xsum.at[i, z], out_grads.at[i, at, :], ws.at[i, k], wr.at[i, k], dev(dz=k)).wait_recv()
        q = out_squares.at[back(z, k, nz)]
        make(q, q, qzs.at[k], qzr.at[k], dev(dz=k)).wait_recv()
    for copy in sent:
        copy.wait_send()


def reduce_all(sizes, part, grads):
    nz, nx, ny, nc = sizes
    rows, width = part.shape[3:]
    mine = grads[0].shape[0]
    cols = width // (nz * nx)
    dma = pltpu.SemaphoreType.DMA
    vmem = pl.BlockSpec(memory_space=pltpu.VMEM)
    return pl.pallas_call(
        functools.partial(reduce_kernel, sizes),
        out_shape=[
            jax.ShapeDtypeStruct((rows, width), BF),
            jax.ShapeDtypeStruct((3, nz * mine, cols), BF),
            jax.ShapeDtypeStruct((nz, 3, 8, mine), F32),
        ],
        in_specs=[vmem] * 4,
        out_specs=[vmem] * 3,
        scratch_shapes=[
            pltpu.VMEM((nz, ny, nc, rows, width), BF),
            pltpu.VMEM((nz, ny, rows, width), BF),
            pltpu.VMEM((nz, ny, rows, width), BF),
            pltpu.VMEM((nz, rows, width), BF),
            pltpu.VMEM((nz, rows, width), BF),
            pltpu.VMEM((3, nz, nx, mine, cols), BF),
            pltpu.VMEM((3, nz, mine, cols), BF),
            pltpu.VMEM((3, 8, mine), F32),
            pltpu.VMEM((nx, 3, 8, mine), F32),
            dma((nz, ny, nc)),
            dma((nz, ny, nc)),
            dma((nz, ny)),
            dma((nz, ny)),
            dma((nz,)),
            dma((nz,)),
            dma((3, nz, nx)),
            dma((3, nz, nx)),
            dma((3, nz)),
            dma((3, nz)),
            dma((nx,)),
            dma((nx,)),
            dma((nz,)),
            dma((nz,)),
        ],
        compiler_params=pltpu.CompilerParams(collective_id=1, has_side_effects=True, vmem_limit_bytes=60 * 1024 * 1024),
    )(part, *grads)


def make_body(fs, tp):
    nz, nx, ny, nc = split_sizes(fs, tp)

    def body(tokens, gate_weight, up_weight, down_weight, out_grad):
        rows, width = tokens.shape
        hid, cols = gate_weight.shape
        inputs, cotangent, w_gate, w_up, w_down = gather_all(
            (nz, nx, ny, nc), tokens, out_grad, (gate_weight, up_weight, down_weight)
        )
        inner = (((1,), (1,)), ((), ()))
        gate = lax.dot_general(inputs, w_gate, inner, preferred_element_type=F32)
        up = lax.dot_general(inputs, w_up, inner, preferred_element_type=F32)
        dhidden = lax.dot_general(cotangent, w_down, inner, preferred_element_type=F32)
        sig = jax.nn.sigmoid(gate)
        silu = gate * sig
        act = (silu * up).astype(BF)
        dgate = (dhidden * up * sig * (1.0 + gate * (1.0 - sig))).astype(BF)
        dup = (dhidden * silu).astype(BF)
        factor = 1.0 / math.sqrt(rows * fs * tp)
        outer = (((0,), (0,)), ((), ()))

        def weight_grad(left, right):
            return (lax.dot_general(left, right, outer, preferred_element_type=F32) * factor).astype(BF)

        grads = (weight_grad(dgate, inputs), weight_grad(dup, inputs), weight_grad(act, cotangent))
        part = jnp.dot(dgate, w_gate, preferred_element_type=F32)
        part = (part + jnp.dot(dup, w_up, preferred_element_type=F32)).astype(BF)
        grad_tokens, grad, squares = reduce_all(
            (nz, nx, ny, nc), part.reshape(nz, ny, nc, rows, width), grads
        )
        grad = grad.astype(F32)
        means = squares[:, :, 0, :].transpose(1, 0, 2).reshape(3, hid) / width
        return (grad_tokens, grad[0], grad[1], grad[2], means[0], means[1], means[2])

    return body


def solution(mesh):
    return jax.shard_map(
        make_body(mesh.shape["fs"], mesh.shape["tp"]),
        mesh=mesh,
        in_specs=(P(("fs", "tp"), None), P("tp", "fs"), P("tp", "fs"), P("tp", "fs"), P(("fs", "tp"), None)),
        out_specs=(
            P(("fs", "tp"), None),
            P("tp", "fs"),
            P("tp", "fs"),
            P("tp", "fs"),
            P("tp"),
            P("tp"),
            P("tp"),
        ),
        check_vma=False,
    )
```
